32 devices in a mesh: sp: 8 (over z, y), tp: 4 (over x, core).
Axes of the slice: x: 2, y: 2, z: 4, core: 2. Of those that a mesh axis runs over, the one named last changes fastest.
Arguments:
- tokens: bfloat16 [1536, 2048], P(('sp', 'tp')), may hold values from -6 to 6
- norm_in: float32 [2048], replicated, may hold values from 0.1 to 1.9
- decay_log: float32 [128, 64], P('tp'), may hold values from -0.034 to -0.00016276042, as said below
- phase: float32 [128, 64], P('tp'), may hold values from -1 to 1
- b_real: float32 [128, 64, 16], P('tp'), may hold values from -1 to 1
- b_imag: float32 [128, 64, 16], P('tp'), may hold values from -1 to 1
- c_real: float32 [128, 16, 64], P('tp'), may hold values from -0.75 to 0.75
- c_imag: float32 [128, 16, 64], P('tp'), may hold values from -0.75 to 0.75
- skip_gain: float32 [2048], P('tp'), may hold values from -6 to 6
- w_value: bfloat16 [2048, 2048], P(None, 'tp'), as said below
- w_gate: bfloat16 [2048, 2048], P(None, 'tp'), may hold values from -0.125 to 0.125
- norm_out: float32 [2048], P('tp'), may hold values from 0.1 to 1.9
Outputs:
- mixed: bfloat16 [1536, 2048], P('sp', 'tp')
The draws below stay inside these ranges and needn't reach their ends.
Inputs may be any that keep to these rules, and one draw needn't show every extreme that they name: `decay_log`: negative real parts of the eigenvalues. `w_value`: weights of the value projection.
All inputs are finite; a program needn't handle non-finite values.
Results may differ from the reference program's by a relative error of at most 0.012.
The reference program's roundings to bfloat16 on the way count: a program that leaves them out, or rounds other values in their place, can miss the bound.
Values may be sent and summed in bfloat16 or wider, within the bound.
No kernel may reach another device: no remote copies, remote signals or barrier semaphores. Data moves between devices by JAX's collectives and lax.ppermute only.
A program may use at most 64 MiB of HBM per device.

```python
import math
import jax
import jax.numpy as jnp
from jax import lax

D = 2048
GROUP = 16
STATE = 64
GROUPS = 128
TOK_DEV = 192
TOKENS = 1536
N_SP = 8


def draw_decay_log(key, part):
    first_key = jax.random.fold_in(key, 11)
    second_key = jax.random.fold_in(key, 12)
    third_key = jax.random.fold_in(key, 13)
    slow_share = 0.5
    slow_flag = jax.random.uniform(first_key, (GROUPS, 1), jnp.float32) < slow_share
    slow_rate = jnp.exp(jax.random.uniform(second_key, (GROUPS, STATE), jnp.float32, math.log(0.25), math.log(2.2))) / TOKENS
    fast_rate = jnp.exp(jax.random.uniform(third_key, (GROUPS, STATE), jnp.float32, math.log(0.0101), math.log(0.0333)))
    return -jnp.where(slow_flag, slow_rate, fast_rate)


def draw_w_value(key, part):
    top_scale = 10.0
    columns = jnp.arange(D, dtype=jnp.float32)
    column_scale = jnp.exp(math.log(top_scale) * columns / D)
    base = jax.random.normal(key, (D, D), jnp.float32) * D ** (-0.5)
    return (base * column_scale[None, :]).astype(jnp.bfloat16)


def block_levels(key, dims, shards, low, top_value):
    def one(dim, shards_of):
        steps = jax.random.uniform(jax.random.fold_in(jax.random.fold_in(key, 6), dim), (shards_of,), jnp.float32, low / len(shards), top_value / len(shards))
        return jnp.repeat(jnp.exp(steps), dims[dim] // shards_of).reshape((-1,) + (1,) * (len(dims) - dim - 1))

    level = one(*shards[0])
    for cut in shards[1:]:
        level = level * one(*cut)
    return level


def centred(rng, dims, spread, bound, cuts=(), kind=jnp.bfloat16):
    result = jax.random.normal(rng, dims, jnp.float32) * spread
    if len(cuts) > 0:
        result = block_levels(rng, dims, cuts, -0.22, 0.18) * result
    return jnp.clip(result, min=-bound, max=bound).astype(kind)


def setup_inputs(seed: int = 0) -> dict:
    splits = jax.random.split(jax.random.key(seed), 13)
    return {
        "tokens": centred(splits[0], (TOKENS, D), 1.0, 6.0, ((0, 32),)),
        "norm_in": jnp.clip(1.0 + 0.18 * jax.random.normal(splits[1], (D,), jnp.float32), 0.1, 1.9),
        "decay_log": draw_decay_log(jax.random.fold_in(splits[12], 71), 0),
        "phase": jnp.clip(jax.random.uniform(splits[3], (GROUPS, STATE), jnp.float32, -1.0, 1.0) * block_levels(splits[3], (GROUPS, STATE), ((0, 4),), -0.4, 0.0), -1.0, 1.0),
        "b_real": centred(splits[4], (GROUPS, STATE, GROUP), (2 * GROUP) ** -0.5, 1.0, ((0, 4),), jnp.float32),
        "b_imag": centred(splits[5], (GROUPS, STATE, GROUP), (2 * GROUP) ** -0.5, 1.0, ((0, 4),), jnp.float32),
        "c_real": centred(splits[6], (GROUPS, GROUP, STATE), STATE ** -0.5, 0.75, ((0, 4),), jnp.float32),
        "c_imag": centred(splits[7], (GROUPS, GROUP, STATE), STATE ** -0.5, 0.75, ((0, 4),), jnp.float32),
        "skip_gain": centred(splits[8], (D,), 1.0, 6.0, ((0, 4),), jnp.float32),
        "w_value": draw_w_value(jax.random.fold_in(splits[12], 71), 0),
        "w_gate": centred(splits[10], (D, D), D ** -0.5, 0.125, ((1, 4),)),
        "norm_out": jnp.clip(1.0 + 0.18 * jax.random.normal(splits[11], (D,), jnp.float32), 0.1, 1.9),
    }


NORM_EPS = 1e-06
HIGHEST_PREC = lax.Precision.HIGHEST

def coefficients(decay_log, phase, b_real, b_imag):
    magnitude = jnp.exp(decay_log)
    bar_re = magnitude * jnp.cos(phase)
    bar_im = magnitude * jnp.sin(phase)
    modulus = decay_log * decay_log + phase * phase
    coef_re = ((bar_re - 1.0) * decay_log + bar_im * phase) / modulus
    coef_im = (bar_im * decay_log - (bar_re - 1.0) * phase) / modulus
    in_re = coef_re[:, :, None] * b_real - coef_im[:, :, None] * b_imag
    in_im = coef_re[:, :, None] * b_imag + coef_im[:, :, None] * b_real
    return (bar_re, bar_im, in_re, in_im)

def prefix_states(drive_re, drive_im, rate_re, rate_im):
    length = drive_re.shape[0]
    stride = 1
    for level in range(max(length - 1, 1).bit_length()):
        padding = jnp.zeros((stride,) + drive_re.shape[1:], jnp.float32)
        moved_re = jnp.concatenate([padding, drive_re[:length - stride]], axis=0)
        moved_im = jnp.concatenate([padding, drive_im[:length - stride]], axis=0)
        drive_re, drive_im = (drive_re + rate_re * moved_re - rate_im * moved_im, drive_im + rate_re * moved_im + rate_im * moved_re)
        rate_re, rate_im = (rate_re * rate_re - rate_im * rate_im, 2.0 * rate_re * rate_im)
        stride = stride * 2
    return (drive_re, drive_im)

def readout(state_re, state_im, c_real, c_imag):
    first = jnp.einsum('tgp,ghp->tgh', state_re, c_real, precision=HIGHEST_PREC)
    second = jnp.einsum('tgp,ghp->tgh', state_im, c_imag, precision=HIGHEST_PREC)
    return first - second

def reference(tokens, norm_in, decay_log, phase, b_real, b_imag, c_real, c_imag, skip_gain, w_value, w_gate, norm_out):
    xf = tokens.astype(jnp.float32)
    normed = (xf * lax.rsqrt(lax.optimization_barrier(jnp.mean(xf * xf, axis=1, keepdims=True)) + NORM_EPS) * norm_in).astype(jnp.bfloat16)
    bar_re, bar_im, bb_re, bb_im = coefficients(decay_log, phase, b_real, b_imag)
    blocks = normed.reshape(N_SP, TOK_DEV, GROUPS, GROUP)
    skip_grid = skip_gain.reshape(GROUPS, GROUP)

    def block_step(carried, block):
        state_re, state_im = carried
        drive = block.astype(jnp.float32)
        in_re = jnp.einsum('tgh,gph->tgp', drive, bb_re, precision=HIGHEST_PREC)
        in_im = jnp.einsum('tgh,gph->tgp', drive, bb_im, precision=HIGHEST_PREC)
        in_re = in_re.at[0].add(bar_re * state_re - bar_im * state_im)
        in_im = in_im.at[0].add(bar_re * state_im + bar_im * state_re)
        all_re, all_im = prefix_states(in_re, in_im, bar_re, bar_im)
        mixed_pre = readout(all_re, all_im, c_real, c_imag) + skip_grid * drive
        z_block = jax.nn.gelu(mixed_pre).reshape(TOK_DEV, D).astype(jnp.bfloat16)
        return ((all_re[-1], all_im[-1]), z_block)
    start_state = (jnp.zeros((GROUPS, STATE), jnp.float32), jnp.zeros((GROUPS, STATE), jnp.float32))
    ignored, z_blocks = lax.scan(block_step, start_state, blocks)
    z_all = z_blocks.reshape(N_SP * TOK_DEV, D)
    projected_value = jnp.dot(z_all, w_value, preferred_element_type=jnp.float32)
    projected_gate = jnp.dot(z_all, w_gate, preferred_element_type=jnp.float32)
    gated = projected_value * jax.nn.sigmoid(projected_gate)
    scale = lax.rsqrt(lax.optimization_barrier(jnp.mean(gated * gated, axis=1, keepdims=True)) + NORM_EPS)
    return (gated * scale * norm_out).astype(jnp.bfloat16)
```

```python
import functools

import jax
import jax.numpy as jnp
from jax import lax
from jax.experimental import pallas as pl
from jax.experimental.pallas import tpu as pltpu
from jax.sharding import PartitionSpec as P

NORM_EPS = 1e-06
SEG = 8
LANES = 128
F32 = jnp.float32
BF16 = jnp.bfloat16
NT_DIMS = (((1,), (1,)), ((), ()))


def iota(shape, dim):
    return lax.broadcasted_iota(jnp.int32, shape, dim)


def cmul(a, b):
    return (a[0] * b[0] - a[1] * b[1], a[0] * b[1] + a[1] * b[0])


def cpow(a, n):
    result = None
    while n:
        if n & 1:
            result = a if result is None else cmul(result, a)
        n >>= 1
        if n:
            a = cmul(a, a)
    return result


def rate(decay, phase):
    magnitude = jnp.exp(decay)
    return (magnitude * jnp.cos(phase), magnitude * jnp.sin(phase))


def row(pair, index):
    shape = (SEG, LANES)
    return tuple(jnp.broadcast_to(part[index : index + 1, :], shape) for part in pair)


def norm_kernel(x_ref, gain_ref, out_ref):
    x = x_ref[...].astype(F32)
    mean = jnp.mean(x * x, axis=1, keepdims=True)
    y = (x * lax.rsqrt(mean + NORM_EPS) * gain_ref[...]).astype(BF16)
    count, _, width = out_ref.shape
    for k in range(count):
        out_ref[k] = y[:, k * width : (k + 1) * width]


def drive_tile(rows, wb_ref, k, part):
    return lax.dot_general(rows, wb_ref[k, part], NT_DIMS, preferred_element_type=F32)


def ends_kernel(u_ref, br_ref, bi_ref, decay_ref, phase_ref, up_ref, wb_ref, init_ref, end_ref, d_ref, e_ref):
    total, width = u_ref.shape
    steps = total // SEG
    tiles, _, states, _ = wb_ref.shape
    per = states // LANES
    group = br_ref.shape[1]
    entries = states * group // LANES
    r, t = iota((total, total), 0), iota((total, total), 1)
    order = (t == (r % SEG) * steps + r // SEG).astype(F32).astype(BF16)
    up_ref[...] = jnp.dot(order, u_ref[...], preferred_element_type=F32).astype(BF16)
    spread = (iota((group, LANES), 1) % group == iota((group, LANES), 0)).astype(F32).astype(BF16)
    mask = iota((states, LANES), 0) // entries == iota((states, LANES), 1) // group
    lam = rate(decay_ref[...], phase_ref[...])
    hop = cpow(lam, steps)
    hops = [hop, cmul(hop, hop)]
    hops.append(cmul(hops[1], hops[1]))
    sub = iota((SEG, LANES), 0)
    for k in range(tiles):
        for part, ref in enumerate((br_ref, bi_ref)):
            rep = jnp.dot(
                ref[k * states : (k + 1) * states, :].astype(BF16), spread, preferred_element_type=F32
            )
            wb_ref[k, part] = jnp.where(mask, rep, 0.0).astype(BF16)
            d_ref[part] = drive_tile(up_ref[:, k * LANES : (k + 1) * LANES], wb_ref, k, part)
        lams = [row(lam, k * per + m) for m in range(per)]
        x = [(d_ref[0, 0:SEG, m * LANES : (m + 1) * LANES], d_ref[1, 0:SEG, m * LANES : (m + 1) * LANES]) for m in range(per)]
        for j in range(1, steps):
            for m in range(per):
                sl = slice(m * LANES, (m + 1) * LANES)
                moved = cmul(lams[m], x[m])
                x[m] = (
                    moved[0] + d_ref[0, j * SEG : (j + 1) * SEG, sl],
                    moved[1] + d_ref[1, j * SEG : (j + 1) * SEG, sl],
                )
        for m in range(per):
            index = k * per + m
            e = x[m]
            for level in range(3):
                d = 1 << level
                back = tuple(jnp.where(sub >= d, pltpu.roll(part, d, 0), 0.0) for part in e)
                add = cmul(row(hops[level], index), back)
                e = (e[0] + add[0], e[1] + add[1])
            pairs = tiles * per
            for part in range(2):
                init_ref[part, index] = jnp.where(sub >= 1, pltpu.roll(e[part], 1, 0), 0.0)
                e_ref[part * pairs + index : part * pairs + index + 1, :] = e[part][SEG - 1 : SEG, :]
    ends = e_ref[...]
    for n in range(end_ref.shape[0]):
        end_ref[n] = ends


def mixer_kernel(
    mine_ref, up_ref, wb_ref, init_ref, end_ref, cr_ref, ci_ref, gdecay_ref, gphase_ref,
    decay_ref, phase_ref, skip_ref, z_ref, d_ref, s_ref, cw_ref, zp_ref,
):
    total, width = up_ref.shape
    steps = total // SEG
    tiles, _, states, _ = wb_ref.shape
    per = states // LANES
    pairs = tiles * per
    entries = cr_ref.shape[1]
    groups = gdecay_ref.shape[0]
    group = cr_ref.shape[0] // groups
    each = LANES // group
    gd, gp = gdecay_ref[...], gphase_ref[...]
    gbar = rate(gd, gp)
    modulus = gd * gd + gp * gp
    coef_re = ((gbar[0] - 1.0) * gd + gbar[1] * gp) / modulus
    coef_im = (gbar[1] * gd - (gbar[0] - 1.0) * gp) / modulus
    lam = rate(decay_ref[...], phase_ref[...])
    hop = cpow(lam, steps)
    hop2 = cmul(hop, hop)
    hop4 = cmul(hop2, hop2)
    whole = cmul(hop4, hop4)

    def join(i, held):
        moved = cmul(whole, held)
        return (moved[0] + end_ref[i, 0:pairs, :], moved[1] + end_ref[i, pairs : 2 * pairs, :])

    nothing = jnp.zeros((pairs, LANES), F32)
    held = lax.fori_loop(0, mine_ref[0], join, (nothing, nothing))
    sub = iota((SEG, LANES), 0)
    for k in range(tiles):
        rows = up_ref[:, k * LANES : (k + 1) * LANES]
        for part in range(2):
            d_ref[part] = drive_tile(rows, wb_ref, k, part)
        cw_ref[...] = jnp.zeros(cw_ref.shape, BF16)
        blank = jnp.zeros((group, entries), F32)
        for q in range(each):
            g = k * each + q
            cr = cr_ref[g * group : (g + 1) * group, :]
            ci = ci_ref[g * group : (g + 1) * group, :]
            fr, fi = coef_re[g : g + 1, :], coef_im[g : g + 1, :]
            per_vreg = LANES // entries
            m, slot = q // per_vreg, q % per_vreg
            for part, value in enumerate((cr * fr - ci * fi, -(cr * fi + ci * fr))):
                wide = jnp.concatenate([value if n == slot else blank for n in range(per_vreg)], axis=1)
                start = part * states + m * LANES
                cw_ref[q * group : (q + 1) * group, start : start + LANES] = wide.astype(BF16)
        lams, x = [], []
        for m in range(per):
            index = k * per + m
            lams.append(row(lam, index))
            power = (jnp.ones((SEG, LANES), F32), jnp.zeros((SEG, LANES), F32))
            for level, value in enumerate((hop, hop2, hop4)):
                bit = (sub >> level) & 1 == 1
                more = cmul(power, row(value, index))
                power = tuple(jnp.where(bit, a, b) for a, b in zip(more, power))
            seed = cmul(power, row(held, index))
            x.append((init_ref[0, index] + seed[0], init_ref[1, index] + seed[1]))
        for j in range(0, steps, 2):
            for m in range(per):
                sl = slice(m * LANES, (m + 1) * LANES)
                two = []
                for i in (j, j + 1):
                    moved = cmul(lams[m], x[m])
                    x[m] = (
                        moved[0] + d_ref[0, i * SEG : (i + 1) * SEG, sl],
                        moved[1] + d_ref[1, i * SEG : (i + 1) * SEG, sl],
                    )
                    two.append(x[m])
                for part in range(2):
                    start = part * states + m * LANES
                    s_ref[j * SEG : (j + 2) * SEG, start : start + LANES] = jnp.concatenate(
                        [two[0][part], two[1][part]], axis=0
                    ).astype(BF16)
        y = lax.dot_general(s_ref[...], cw_ref[...], NT_DIMS, preferred_element_type=F32)
        y = y + skip_ref[:, k * LANES : (k + 1) * LANES] * rows.astype(F32)
        zp_ref[:, k * LANES : (k + 1) * LANES] = jax.nn.gelu(y).astype(BF16)
    t, r = iota((total, total), 0), iota((total, total), 1)
    order = (t == (r % SEG) * steps + r // SEG).astype(F32).astype(BF16)
    z_ref[...] = jnp.dot(order, zp_ref[...], preferred_element_type=F32).astype(BF16)


def on_device(
    tokens, norm_in, decay_log, phase, b_real, b_imag, c_real, c_imag, skip_gain, w_value, w_gate, norm_out
):
    n_sp, n_tp = lax.axis_size("sp"), lax.axis_size("tp")
    rows_own, features = tokens.shape
    width = features // n_tp
    total = rows_own * n_tp
    groups, entries = decay_log.shape
    group = width // groups
    tiles = width // LANES
    states = LANES // group * entries
    pairs = groups * entries // LANES
    shape = jax.ShapeDtypeStruct
    limit = pltpu.CompilerParams(vmem_limit_bytes=40 * 1024 * 1024)
    normed = pl.pallas_call(norm_kernel, out_shape=shape((n_tp, rows_own, width), BF16))(
        tokens, norm_in.reshape(1, features)
    )
    mine = lax.all_to_all(normed, "tp", split_axis=0, concat_axis=0, tiled=True)
    u = mine.reshape(total, width)
    lane_decay = decay_log.reshape(pairs, LANES)
    lane_phase = phase.reshape(pairs, LANES)
    up, wb, init, ends = pl.pallas_call(
        ends_kernel,
        out_shape=(
            shape((total, width), BF16),
            shape((tiles, 2, states, LANES), BF16),
            shape((2, pairs, SEG, LANES), F32),
            shape((n_sp, 2 * pairs, LANES), F32),
        ),
        scratch_shapes=[pltpu.VMEM((2, total, states), F32), pltpu.VMEM((2 * pairs, LANES), F32)],
        compiler_params=limit,
    )(
        u,
        b_real.reshape(groups * entries, group),
        b_imag.reshape(groups * entries, group),
        lane_decay,
        lane_phase,
    )
    others = lax.all_to_all(ends, "sp", split_axis=0, concat_axis=0, tiled=True)
    vmem = pl.BlockSpec(memory_space=pltpu.VMEM)
    z = pl.pallas_call(
        mixer_kernel,
        out_shape=shape((total, width), BF16),
        in_specs=[pl.BlockSpec(memory_space=pltpu.SMEM)] + [vmem] * 11,
        scratch_shapes=[
            pltpu.VMEM((2, total, states), F32),
            pltpu.VMEM((total, 2 * states), BF16),
            pltpu.VMEM((LANES, 2 * states), BF16),
            pltpu.VMEM((total, width), BF16),
        ],
        compiler_params=limit,
    )(
        lax.axis_index("sp").astype(jnp.int32).reshape(1),
        up,
        wb,
        init,
        others,
        c_real.reshape(width, entries),
        c_imag.reshape(width, entries),
        decay_log,
        phase,
        lane_decay,
        lane_phase,
        skip_gain.reshape(1, width),
    )
    z_all = lax.all_gather(z, "tp", axis=1, tiled=True)
    value = jnp.dot(z_all, w_value, preferred_element_type=F32)
    gate = jnp.dot(z_all, w_gate, preferred_element_type=F32)
    gated = value * jax.nn.sigmoid(gate)
    squares = lax.psum(jnp.sum(gated * gated, axis=1), "tp")
    scale = lax.rsqrt(squares / features + NORM_EPS)
    return (gated * scale[:, None] * norm_out).astype(BF16)


def solution(mesh):
    placed = (
        P(("sp", "tp"), None),
        P(),
        P("tp", None),
        P("tp", None),
        P("tp", None, None),
        P("tp", None, None),
        P("tp", None, None),
        P("tp", None, None),
        P("tp"),
        P(None, "tp"),
        P(None, "tp"),
        P("tp"),
    )
    return jax.shard_map(on_device, mesh=mesh, in_specs=placed, out_specs=P("sp", "tp"), check_vma=False)
```

```python
import jax
import jax.numpy as jnp
from jax import lax
from jax.experimental import pallas as pl
from jax.experimental.pallas import tpu as pltpu
from jax.sharding import PartitionSpec as P

NORM_EPS = 1e-06
SEG = 8
LANES = 128
TABLES = 5
F32 = jnp.float32
BF16 = jnp.bfloat16
NT_DIMS = (((1,), (1,)), ((), ()))


def iota(shape, dim):
    return lax.broadcasted_iota(jnp.int32, shape, dim)


def cmul(a, b):
    return (a[0] * b[0] - a[1] * b[1], a[0] * b[1] + a[1] * b[0])


def cpow(a, n):
    result = None
    while n:
        if n & 1:
            result = a if result is None else cmul(result, a)
        n >>= 1
        if n:
            a = cmul(a, a)
    return result


def rate(decay, phase):
    magnitude = jnp.exp(decay)
    return (magnitude * jnp.cos(phase), magnitude * jnp.sin(phase))


def wide_row(pair, index):
    shape = (SEG, LANES)
    return tuple(jnp.broadcast_to(part[index : index + 1, :], shape) for part in pair)


def table_row(tab_ref, power, index):
    shape = (SEG, LANES)
    return tuple(
        jnp.broadcast_to(tab_ref[2 * power + part, index : index + 1, :], shape) for part in range(2)
    )


def forward_order(total):
    steps = total // SEG
    r, t = iota((total, total), 0), iota((total, total), 1)
    return (t == (r % SEG) * steps + r // SEG).astype(F32).astype(BF16)


def place(ref, k, q, part, value):
    group, entries = value.shape
    fits = LANES // entries
    m, slot = q // fits, q % fits
    blank = jnp.zeros(value.shape, F32)
    wide = jnp.concatenate([value if n == slot else blank for n in range(fits)], axis=1)
    start = part * (ref.shape[2] // 2) + m * LANES
    ref[k, q * group : (q + 1) * group, start : start + LANES] = wide.astype(BF16)


def fill_tables(tab_ref, decay_ref, phase_ref, steps):
    fits = LANES // decay_ref.shape[1]
    pairs = decay_ref.shape[0] // fits
    lined = [
        jnp.concatenate([ref[pl.ds(n, pairs, stride=fits), :] for n in range(fits)], axis=1)
        for ref in (decay_ref, phase_ref)
    ]
    value = rate(*lined)
    for power in range(TABLES):
        for part in range(2):
            tab_ref[2 * power + part] = value[part]
        value = cpow(value, steps) if power == 0 else cmul(value, value)


def fetch(sources, targets, sem):
    copies = [pltpu.make_async_copy(s, t, sem.at[n]) for n, (s, t) in enumerate(zip(sources, targets))]
    for copy in copies:
        copy.start()
    return copies


def norm_kernel(x_ref, gain_ref, out_ref):
    x = x_ref[...].astype(F32)
    mean = jnp.mean(x * x, axis=1, keepdims=True)
    y = (x * lax.rsqrt(mean + NORM_EPS) * gain_ref[...]).astype(BF16)
    count, _, width = out_ref.shape
    for k in range(count):
        out_ref[k] = y[:, k * width : (k + 1) * width]


def fill_inputs(wb_ref, br_ref, bi_ref, group):
    wb_ref[...] = jnp.zeros(wb_ref.shape, BF16)
    each = LANES // group
    for k in range(wb_ref.shape[0]):
        for q in range(each):
            start = (k * each + q) * group
            for part, ref in enumerate((br_ref, bi_ref)):
                place(wb_ref, k, q, part, ref[start : start + group, :])


def weights_kernel(steps, br_hbm, bi_hbm, decay_hbm, phase_hbm, wb_ref, tab_ref, br_ref, bi_ref, decay_ref, phase_ref, sem):
    copies = fetch((decay_hbm, phase_hbm, br_hbm, bi_hbm), (decay_ref, phase_ref, br_ref, bi_ref), sem)
    copies[0].wait()
    copies[1].wait()
    fill_tables(tab_ref, decay_ref, phase_ref, steps)
    copies[2].wait()
    copies[3].wait()
    fill_inputs(wb_ref, br_ref, bi_ref, br_ref.shape[0] // decay_ref.shape[0])


def lanes_of(d_ref, part, j, m):
    half = d_ref.shape[1] // 2
    start = part * half + m * LANES
    return d_ref[j * SEG : (j + 1) * SEG, start : start + LANES]


def ends_kernel(u_ref, wb_ref, tab_ref, up_hbm, init_hbm, end_hbm, up_ref, init_ref, end_ref, d_ref, e_ref, sem):
    total = u_ref.shape[0]
    steps = total // SEG
    tiles, _, both = wb_ref.shape
    per = both // 2 // LANES
    pairs = tiles * per
    up_ref[...] = jnp.dot(forward_order(total), u_ref[...], preferred_element_type=F32).astype(BF16)
    first = fetch((up_ref,), (up_hbm,), sem)
    sub = iota((SEG, LANES), 0)
    for k in range(tiles):
        d_ref[...] = jnp.dot(up_ref[:, k * LANES : (k + 1) * LANES], wb_ref[k], preferred_element_type=F32)
        lams = [table_row(tab_ref, 0, k * per + m) for m in range(per)]
        x = [(lanes_of(d_ref, 0, 0, m), lanes_of(d_ref, 1, 0, m)) for m in range(per)]
        for j in range(1, steps):
            for m in range(per):
                moved = cmul(lams[m], x[m])
                x[m] = tuple(moved[part] + lanes_of(d_ref, part, j, m) for part in range(2))
        for m in range(per):
            index = k * per + m
            e = x[m]
            for level in range(3):
                d = 1 << level
                back = tuple(jnp.where(sub >= d, pltpu.roll(part, d, 0), 0.0) for part in e)
                add = cmul(table_row(tab_ref, 1 + level, index), back)
                e = (e[0] + add[0], e[1] + add[1])
            for part in range(2):
                init_ref[part, index] = jnp.where(sub >= 1, pltpu.roll(e[part], 1, 0), 0.0)
                e_ref[part * pairs + index : part * pairs + index + 1, :] = e[part][SEG - 1 : SEG, :]
    ends = e_ref[...]
    for n in range(end_ref.shape[0]):
        end_ref[n] = ends
    last = fetch((end_ref, init_ref), (end_hbm, init_hbm), sem.at[1:3])
    for copy in first + last:
        copy.wait()


def local_kernel(
    up_hbm, init_hbm, br_hbm, bi_hbm, cr_hbm, ci_hbm, decay_hbm, phase_hbm, skip_hbm,
    y_hbm, cw_ref, tab_ref,
    up_ref, init_ref, br_ref, bi_ref, cr_ref, ci_ref, decay_ref, phase_ref, skip_ref,
    y_ref, wb_ref, d_ref, s_ref, sem,
):
    copies = fetch(
        (up_hbm, init_hbm, br_hbm, bi_hbm, cr_hbm, ci_hbm, decay_hbm, phase_hbm, skip_hbm),
        (up_ref, init_ref, br_ref, bi_ref, cr_ref, ci_ref, decay_ref, phase_ref, skip_ref),
        sem,
    )
    for copy in copies:
        copy.wait()
    total = up_ref.shape[0]
    steps = total // SEG
    groups = decay_ref.shape[0]
    group = br_ref.shape[0] // groups
    each = LANES // group
    tiles, _, both = wb_ref.shape
    per = both // 2 // LANES
    fill_tables(tab_ref, decay_ref, phase_ref, steps)
    fill_inputs(wb_ref, br_ref, bi_ref, group)
    gd, gp = decay_ref[...], phase_ref[...]
    gbar = rate(gd, gp)
    modulus = gd * gd + gp * gp
    coef_re = ((gbar[0] - 1.0) * gd + gbar[1] * gp) / modulus
    coef_im = (gbar[1] * gd - (gbar[0] - 1.0) * gp) / modulus
    cw_ref[...] = jnp.zeros(cw_ref.shape, BF16)
    for k in range(tiles):
        for q in range(each):
            g = k * each + q
            cr = cr_ref[g * group : (g + 1) * group, :]
            ci = ci_ref[g * group : (g + 1) * group, :]
            fr, fi = coef_re[g : g + 1, :], coef_im[g : g + 1, :]
            place(cw_ref, k, q, 0, cr * fr - ci * fi)
            place(cw_ref, k, q, 1, -(cr * fi + ci * fr))
        rows = up_ref[:, k * LANES : (k + 1) * LANES]
        d_ref[...] = jnp.dot(rows, wb_ref[k], preferred_element_type=F32)
        lams = [table_row(tab_ref, 0, k * per + m) for m in range(per)]
        x = [(init_ref[0, k * per + m], init_ref[1, k * per + m]) for m in range(per)]

        def step(j, m):
            moved = cmul(lams[m], x[m])
            x[m] = tuple(moved[part] + lanes_of(d_ref, part, j, m) for part in range(2))
            return x[m]

        roll_states(s_ref, steps, per, step)
        y = lax.dot_general(s_ref[...], cw_ref[k], NT_DIMS, preferred_element_type=F32)
        y_ref[:, k * LANES : (k + 1) * LANES] = y + skip_ref[:, k * LANES : (k + 1) * LANES] * rows.astype(F32)
    last = pltpu.make_async_copy(y_ref, y_hbm, sem.at[9])
    last.start()
    last.wait()


def roll_states(s_ref, steps, per, step):
    half = s_ref.shape[1] // 2
    for j in range(0, steps, 2):
        for m in range(per):
            two = [step(j, m), step(j + 1, m)]
            for part in range(2):
                start = part * half + m * LANES
                s_ref[j * SEG : (j + 2) * SEG, start : start + LANES] = jnp.concatenate(
                    [two[0][part], two[1][part]], axis=0
                ).astype(BF16)


def carry_kernel(mine_ref, end_ref, y_hbm, cw_ref, tab_ref, z_ref, y_ref, s_ref, zp_ref, sem):
    arriving = pltpu.make_async_copy(y_hbm, y_ref, sem)
    arriving.start()
    total = y_ref.shape[0]
    steps = total // SEG
    tiles, _, both = cw_ref.shape
    per = both // 2 // LANES
    pairs = tiles * per
    whole = (tab_ref[2 * TABLES - 2], tab_ref[2 * TABLES - 1])

    def join(i, held):
        moved = cmul(whole, held)
        return (moved[0] + end_ref[i, 0:pairs, :], moved[1] + end_ref[i, pairs : 2 * pairs, :])

    nothing = jnp.zeros((pairs, LANES), F32)
    held = lax.fori_loop(0, mine_ref[0], join, (nothing, nothing))
    sub = iota((SEG, LANES), 0)
    for k in range(tiles):
        lams, x = [], []
        for m in range(per):
            index = k * per + m
            lams.append(table_row(tab_ref, 0, index))
            seed = wide_row(held, index)
            for level in range(3):
                bit = (sub >> level) & 1 == 1
                more = cmul(seed, table_row(tab_ref, 1 + level, index))
                seed = tuple(jnp.where(bit, a, b) for a, b in zip(more, seed))
            x.append(seed)

        def step(j, m):
            x[m] = cmul(lams[m], x[m])
            return x[m]

        roll_states(s_ref, steps, per, step)
        sl = slice(k * LANES, (k + 1) * LANES)
        y = lax.dot_general(s_ref[...], cw_ref[k], NT_DIMS, preferred_element_type=F32)
        if k == 0:
            arriving.wait()
        zp_ref[:, sl] = jax.nn.gelu(y + y_ref[:, sl]).astype(BF16)
    t, r = iota((total, total), 0), iota((total, total), 1)
    back = (r == (t % steps) * SEG + t // steps).astype(F32).astype(BF16)
    z_ref[...] = jnp.dot(back, zp_ref[...], preferred_element_type=F32).astype(BF16)


def on_device(
    tokens, norm_in, decay_log, phase, b_real, b_imag, c_real, c_imag, skip_gain, w_value, w_gate, norm_out
):
    n_sp, n_tp = lax.axis_size("sp"), lax.axis_size("tp")
    rows_own, features = tokens.shape
    width = features // n_tp
    total = rows_own * n_tp
    groups, entries = decay_log.shape
    group = width // groups
    tiles = width // LANES
    states = LANES // group * entries
    pairs = groups * entries // LANES
    shape = jax.ShapeDtypeStruct
    limit = pltpu.CompilerParams(vmem_limit_bytes=24 * 1024 * 1024)
    vmem = pl.BlockSpec(memory_space=pltpu.VMEM)
    smem = pl.BlockSpec(memory_space=pltpu.SMEM)
    hbm = pl.BlockSpec(memory_space=pltpu.HBM)
    wide = pltpu.VMEM((width, entries), F32)
    flat = pltpu.VMEM((groups, entries), F32)
    rows_t = ((total, width), BF16)
    init_t = ((2, pairs, SEG, LANES), F32)
    y_t = ((total, width), F32)
    ends_t = ((n_sp, 2 * pairs, LANES), F32)
    block_t = ((tiles, LANES, 2 * states), BF16)
    tab_t = ((2 * TABLES, pairs, LANES), F32)

    def held(t):
        return pltpu.VMEM(*t)

    def far(*arrays):
        return [pltpu.with_memory_space_constraint(a, pltpu.HBM) for a in arrays]

    b_re = b_real.transpose(0, 2, 1).reshape(width, entries)
    b_im = b_imag.transpose(0, 2, 1).reshape(width, entries)
    normed = pl.pallas_call(norm_kernel, out_shape=shape((n_tp, rows_own, width), BF16), name="norm")(
        tokens, norm_in.reshape(1, features)
    )
    mine = lax.all_to_all(normed, "tp", split_axis=0, concat_axis=0, tiled=True)
    u = mine.reshape(total, width)
    wb, tab = pl.pallas_call(
        lambda *refs: weights_kernel(total // SEG, *refs),
        out_shape=(pltpu.VMEM(*block_t), pltpu.VMEM(*tab_t)),
        in_specs=[hbm] * 4,
        scratch_shapes=[wide, wide, flat, flat, pltpu.SemaphoreType.DMA((4,))],
        compiler_params=limit,
        name="weights",
    )(*far(b_re, b_im, decay_log, phase))
    up, init, ends = pl.pallas_call(
        ends_kernel,
        out_shape=(pltpu.HBM(*rows_t), pltpu.HBM(*init_t), pltpu.HBM(*ends_t)),
        out_specs=(hbm, hbm, hbm),
        scratch_shapes=[
            held(rows_t),
            held(init_t),
            held(ends_t),
            pltpu.VMEM((total, 2 * states), F32),
            pltpu.VMEM((2 * pairs, LANES), F32),
            pltpu.SemaphoreType.DMA((3,)),
        ],
        compiler_params=limit,
        name="ends",
    )(u, wb, tab)
    others = lax.all_to_all(ends, "sp", split_axis=0, concat_axis=0, tiled=True)
    y, cw, tab2 = pl.pallas_call(
        local_kernel,
        out_shape=(pltpu.HBM(*y_t), pltpu.VMEM(*block_t), pltpu.VMEM(*tab_t)),
        out_specs=(hbm, vmem, vmem),
        in_specs=[hbm] * 9,
        scratch_shapes=[
            held(rows_t),
            held(init_t),
            wide,
            wide,
            wide,
            wide,
            flat,
            flat,
            pltpu.VMEM((1, width), F32),
            held(y_t),
            held(block_t),
            pltpu.VMEM((total, 2 * states), F32),
            pltpu.VMEM((total, 2 * states), BF16),
            pltpu.SemaphoreType.DMA((10,)),
        ],
        compiler_params=limit,
        name="local",
    )(
        *far(
            up,
            init,
            b_re,
            b_im,
            c_real.reshape(width, entries),
            c_imag.reshape(width, entries),
            decay_log,
            phase,
            skip_gain.reshape(1, width),
        )
    )
    z = pl.pallas_call(
        carry_kernel,
        out_shape=shape(*rows_t),
        in_specs=[smem, vmem, hbm, vmem, vmem],
        scratch_shapes=[
            held(y_t),
            pltpu.VMEM((total, 2 * states), BF16),
            held(rows_t),
            pltpu.SemaphoreType.DMA,
        ],
        compiler_params=limit,
        name="carry",
    )(lax.axis_index("sp").astype(jnp.int32).reshape(1), others, *far(y), cw, tab2)
    z_all = lax.all_gather(z, "tp", axis=1, tiled=True)
    value = jnp.dot(z_all, w_value, preferred_element_type=F32)
    gate = jnp.dot(z_all, w_gate, preferred_element_type=F32)
    gated = value * jax.nn.sigmoid(gate)
    squares = lax.psum(jnp.sum(gated * gated, axis=1), "tp")
    scale = lax.rsqrt(squares / features + NORM_EPS)
    return (gated * scale[:, None] * norm_out).astype(BF16)


def solution(mesh):
    placed = (
        P(("sp", "tp"), None),
        P(),
        P("tp", None),
        P("tp", None),
        P("tp", None, None),
        P("tp", None, None),
        P("tp", None, None),
        P("tp", None, None),
        P("tp"),
        P(None, "tp"),
        P(None, "tp"),
        P("tp"),
    )
    return jax.shard_map(on_device, mesh=mesh, in_specs=placed, out_specs=P("sp", "tp"), check_vma=False)
```

```python
import jax
import jax.numpy as jnp
from jax import lax
from jax.experimental import pallas as pl
from jax.experimental.pallas import tpu as pltpu
from jax.sharding import PartitionSpec as P

NORM_EPS = 1e-06
SEG = 8
LANES = 128
TABLES = 5
F32 = jnp.float32
BF16 = jnp.bfloat16
NT_DIMS = (((1,), (1,)), ((), ()))


def iota(shape, dim):
    return lax.broadcasted_iota(jnp.int32, shape, dim)


def cmul(a, b):
    return (a[0] * b[0] - a[1] * b[1], a[0] * b[1] + a[1] * b[0])


def cpow(a, n):
    result = None
    while n:
        if n & 1:
            result = a if result is None else cmul(result, a)
        n >>= 1
        if n:
            a = cmul(a, a)
    return result


def rate(decay, phase):
    magnitude = jnp.exp(decay)
    return (magnitude * jnp.cos(phase), magnitude * jnp.sin(phase))


def wide_row(pair, index):
    shape = (SEG, LANES)
    return tuple(jnp.broadcast_to(part[index : index + 1, :], shape) for part in pair)


def table_row(tab_ref, power, index):
    shape = (SEG, LANES)
    return tuple(
        jnp.broadcast_to(tab_ref[2 * power + part, index : index + 1, :], shape) for part in range(2)
    )


def forward_order(total, rows_own, source):
    steps = total // SEG
    r, c = iota((total, rows_own), 0), iota((total, rows_own), 1)
    return (source * rows_own + c == (r % SEG) * steps + r // SEG).astype(F32).astype(BF16)


def place(ref, k, q, part, value):
    group, entries = value.shape
    fits = LANES // entries
    m, slot = q // fits, q % fits
    blank = jnp.zeros(value.shape, F32)
    wide = jnp.concatenate([value if n == slot else blank for n in range(fits)], axis=1)
    start = part * (ref.shape[2] // 2) + m * LANES
    ref[k, q * group : (q + 1) * group, start : start + LANES] = wide.astype(BF16)


def fill_tables(tab_ref, decay_ref, phase_ref, steps):
    fits = LANES // decay_ref.shape[1]
    pairs = decay_ref.shape[0] // fits
    lined = [
        jnp.concatenate([ref[pl.ds(n, pairs, stride=fits), :] for n in range(fits)], axis=1)
        for ref in (decay_ref, phase_ref)
    ]
    value = rate(*lined)
    for power in range(TABLES):
        for part in range(2):
            tab_ref[2 * power + part] = value[part]
        value = cpow(value, steps) if power == 0 else cmul(value, value)


def fetch(sources, targets, sem):
    copies = [pltpu.make_async_copy(s, t, sem.at[n]) for n, (s, t) in enumerate(zip(sources, targets))]
    for copy in copies:
        copy.start()
    return copies


def norm_kernel(mine_ref, x_ref, gain_ref, *out_refs):
    x = x_ref[...].astype(F32)
    mean = jnp.mean(x * x, axis=1, keepdims=True)
    y = (x * lax.rsqrt(mean + NORM_EPS) * gain_ref[...]).astype(BF16)
    mine = mine_ref[0]
    width = out_refs[0].shape[1]
    for c in range(len(out_refs)):
        for m, out_ref in enumerate(out_refs):

            @pl.when((mine ^ m) == c)
            def _():
                out_ref[...] = y[:, c * width : (c + 1) * width]


def fill_inputs(wb_ref, br_ref, bi_ref, group):
    wb_ref[...] = jnp.zeros(wb_ref.shape, BF16)
    each = LANES // group
    for k in range(wb_ref.shape[0]):
        for q in range(each):
            start = (k * each + q) * group
            for part, ref in enumerate((br_ref, bi_ref)):
                place(wb_ref, k, q, part, ref[start : start + group, :])


def weights_kernel(steps, br_hbm, bi_hbm, decay_hbm, phase_hbm, wb_ref, tab_ref, br_ref, bi_ref, decay_ref, phase_ref, sem):
    copies = fetch((decay_hbm, phase_hbm, br_hbm, bi_hbm), (decay_ref, phase_ref, br_ref, bi_ref), sem)
    copies[0].wait()
    copies[1].wait()
    fill_tables(tab_ref, decay_ref, phase_ref, steps)
    copies[2].wait()
    copies[3].wait()
    fill_inputs(wb_ref, br_ref, bi_ref, br_ref.shape[0] // decay_ref.shape[0])


def lanes_of(d_ref, part, j, m):
    half = d_ref.shape[1] // 2
    start = part * half + m * LANES
    return d_ref[j * SEG : (j + 1) * SEG, start : start + LANES]


def ends_kernel(count, mine_ref, *refs):
    u_refs = refs[:count]
    wb_ref, tab_ref, up_hbm, init_hbm, end_hbm, up_ref, init_ref, end_ref, d_ref, e_ref, sem = refs[count:]
    total = up_ref.shape[0]
    rows_own = total // count
    steps = total // SEG
    tiles, _, both = wb_ref.shape
    per = both // 2 // LANES
    pairs = tiles * per
    ordered = None
    for m, u_ref in enumerate(u_refs):
        order = forward_order(total, rows_own, mine_ref[0] ^ m)
        part = jnp.dot(order, u_ref[...], preferred_element_type=F32)
        ordered = part if ordered is None else ordered + part
    up_ref[...] = ordered.astype(BF16)
    first = fetch((up_ref,), (up_hbm,), sem)
    sub = iota((SEG, LANES), 0)
    for k in range(tiles):
        d_ref[...] = jnp.dot(up_ref[:, k * LANES : (k + 1) * LANES], wb_ref[k], preferred_element_type=F32)
        lams = [table_row(tab_ref, 0, k * per + m) for m in range(per)]
        x = [(lanes_of(d_ref, 0, 0, m), lanes_of(d_ref, 1, 0, m)) for m in range(per)]
        for j in range(1, steps):
            for m in range(per):
                moved = cmul(lams[m], x[m])
                x[m] = tuple(moved[part] + lanes_of(d_ref, part, j, m) for part in range(2))
        for m in range(per):
            index = k * per + m
            e = x[m]
            for level in range(3):
                d = 1 << level
                back = tuple(jnp.where(sub >= d, pltpu.roll(part, d, 0), 0.0) for part in e)
                add = cmul(table_row(tab_ref, 1 + level, index), back)
                e = (e[0] + add[0], e[1] + add[1])
            for part in range(2):
                init_ref[part, index] = jnp.where(sub >= 1, pltpu.roll(e[part], 1, 0), 0.0)
                e_ref[part * pairs + index : part * pairs + index + 1, :] = e[part][SEG - 1 : SEG, :]
    ends = e_ref[...]
    for n in range(end_ref.shape[0]):
        end_ref[n] = ends
    last = fetch((end_ref, init_ref), (end_hbm, init_hbm), sem.at[1:3])
    for copy in first + last:
        copy.wait()


def local_kernel(
    up_hbm, init_hbm, br_hbm, bi_hbm, cr_hbm, ci_hbm, decay_hbm, phase_hbm, skip_hbm,
    y_hbm, cw_ref, tab_ref,
    up_ref, init_ref, br_ref, bi_ref, cr_ref, ci_ref, decay_ref, phase_ref, skip_ref,
    y_ref, wb_ref, d_ref, s_ref, sem,
):
    copies = fetch(
        (up_hbm, init_hbm, br_hbm, bi_hbm, cr_hbm, ci_hbm, decay_hbm, phase_hbm, skip_hbm),
        (up_ref, init_ref, br_ref, bi_ref, cr_ref, ci_ref, decay_ref, phase_ref, skip_ref),
        sem,
    )
    for copy in copies:
        copy.wait()
    total = up_ref.shape[0]
    steps = total // SEG
    groups = decay_ref.shape[0]
    group = br_ref.shape[0] // groups
    each = LANES // group
    tiles, _, both = wb_ref.shape
    per = both // 2 // LANES
    fill_tables(tab_ref, decay_ref, phase_ref, steps)
    fill_inputs(wb_ref, br_ref, bi_ref, group)
    gd, gp = decay_ref[...], phase_ref[...]
    gbar = rate(gd, gp)
    modulus = gd * gd + gp * gp
    coef_re = ((gbar[0] - 1.0) * gd + gbar[1] * gp) / modulus
    coef_im = (gbar[1] * gd - (gbar[0] - 1.0) * gp) / modulus
    cw_ref[...] = jnp.zeros(cw_ref.shape, BF16)
    for k in range(tiles):
        for q in range(each):
            g = k * each + q
            cr = cr_ref[g * group : (g + 1) * group, :]
            ci = ci_ref[g * group : (g + 1) * group, :]
            fr, fi = coef_re[g : g + 1, :], coef_im[g : g + 1, :]
            place(cw_ref, k, q, 0, cr * fr - ci * fi)
            place(cw_ref, k, q, 1, -(cr * fi + ci * fr))
        rows = up_ref[:, k * LANES : (k + 1) * LANES]
        d_ref[...] = jnp.dot(rows, wb_ref[k], preferred_element_type=F32)
        lams = [table_row(tab_ref, 0, k * per + m) for m in range(per)]
        x = [(init_ref[0, k * per + m], init_ref[1, k * per + m]) for m in range(per)]

        def step(j, m):
            moved = cmul(lams[m], x[m])
            x[m] = tuple(moved[part] + lanes_of(d_ref, part, j, m) for part in range(2))
            return x[m]

        roll_states(s_ref, steps, per, step)
        y = lax.dot_general(s_ref[...], cw_ref[k], NT_DIMS, preferred_element_type=F32)
        y_ref[:, k * LANES : (k + 1) * LANES] = y + skip_ref[:, k * LANES : (k + 1) * LANES] * rows.astype(F32)
    last = pltpu.make_async_copy(y_ref, y_hbm, sem.at[9])
    last.start()
    last.wait()


def roll_states(s_ref, steps, per, step):
    half = s_ref.shape[1] // 2
    for j in range(0, steps, 2):
        for m in range(per):
            two = [step(j, m), step(j + 1, m)]
            for part in range(2):
                start = part * half + m * LANES
                s_ref[j * SEG : (j + 2) * SEG, start : start + LANES] = jnp.concatenate(
                    [two[0][part], two[1][part]], axis=0
                ).astype(BF16)


def carry_kernel(mine_ref, end_ref, y_hbm, cw_ref, tab_ref, z_ref, y_ref, s_ref, zp_ref, sem):
    arriving = pltpu.make_async_copy(y_hbm, y_ref, sem)
    arriving.start()
    total = y_ref.shape[0]
    steps = total // SEG
    tiles, _, both = cw_ref.shape
    per = both // 2 // LANES
    pairs = tiles * per
    whole = (tab_ref[2 * TABLES - 2], tab_ref[2 * TABLES - 1])

    def join(i, held):
        moved = cmul(whole, held)
        return (moved[0] + end_ref[i, 0:pairs, :], moved[1] + end_ref[i, pairs : 2 * pairs, :])

    nothing = jnp.zeros((pairs, LANES), F32)
    held = lax.fori_loop(0, mine_ref[0], join, (nothing, nothing))
    sub = iota((SEG, LANES), 0)
    for k in range(tiles):
        lams, x = [], []
        for m in range(per):
            index = k * per + m
            lams.append(table_row(tab_ref, 0, index))
            seed = wide_row(held, index)
            for level in range(3):
                bit = (sub >> level) & 1 == 1
                more = cmul(seed, table_row(tab_ref, 1 + level, index))
                seed = tuple(jnp.where(bit, a, b) for a, b in zip(more, seed))
            x.append(seed)

        def step(j, m):
            x[m] = cmul(lams[m], x[m])
            return x[m]

        roll_states(s_ref, steps, per, step)
        sl = slice(k * LANES, (k + 1) * LANES)
        y = lax.dot_general(s_ref[...], cw_ref[k], NT_DIMS, preferred_element_type=F32)
        if k == 0:
            arriving.wait()
        zp_ref[:, sl] = jax.nn.gelu(y + y_ref[:, sl]).astype(BF16)
    t, r = iota((total, total), 0), iota((total, total), 1)
    back = (r == (t % steps) * SEG + t // steps).astype(F32).astype(BF16)
    z_ref[...] = jnp.dot(back, zp_ref[...], preferred_element_type=F32).astype(BF16)


def on_device(
    tokens, norm_in, decay_log, phase, b_real, b_imag, c_real, c_imag, skip_gain, w_value, w_gate, norm_out
):
    n_sp, n_tp = lax.axis_size("sp"), lax.axis_size("tp")
    rows_own, features = tokens.shape
    width = features // n_tp
    total = rows_own * n_tp
    groups, entries = decay_log.shape
    group = width // groups
    tiles = width // LANES
    states = LANES // group * entries
    pairs = groups * entries // LANES
    shape = jax.ShapeDtypeStruct
    limit = pltpu.CompilerParams(vmem_limit_bytes=24 * 1024 * 1024)
    vmem = pl.BlockSpec(memory_space=pltpu.VMEM)
    smem = pl.BlockSpec(memory_space=pltpu.SMEM)
    hbm = pl.BlockSpec(memory_space=pltpu.HBM)
    wide = pltpu.VMEM((width, entries), F32)
    flat = pltpu.VMEM((groups, entries), F32)
    rows_t = ((total, width), BF16)
    init_t = ((2, pairs, SEG, LANES), F32)
    y_t = ((total, width), F32)
    ends_t = ((n_sp, 2 * pairs, LANES), F32)
    block_t = ((tiles, LANES, 2 * states), BF16)
    tab_t = ((2 * TABLES, pairs, LANES), F32)

    def held(t):
        return pltpu.VMEM(*t)

    def far(*arrays):
        return [pltpu.with_memory_space_constraint(a, pltpu.HBM) for a in arrays]

    b_re = b_real.transpose(0, 2, 1).reshape(width, entries)
    b_im = b_imag.transpose(0, 2, 1).reshape(width, entries)
    tp_mine = lax.axis_index("tp").astype(jnp.int32).reshape(1)

    def partner(x, m):
        return lax.ppermute(x, "tp", [(i, i ^ m) for i in range(n_tp)])

    pieces = pl.pallas_call(
        norm_kernel,
        out_shape=(pltpu.VMEM((rows_own, width), BF16),) + (shape((rows_own, width), BF16),) * (n_tp - 1),
        in_specs=[smem, vmem, vmem],
        name="norm",
    )(tp_mine, tokens, norm_in.reshape(1, features))
    pieces = [piece if m == 0 else partner(piece, m) for m, piece in enumerate(pieces)]
    wb, tab = pl.pallas_call(
        lambda *refs: weights_kernel(total // SEG, *refs),
        out_shape=(pltpu.VMEM(*block_t), pltpu.VMEM(*tab_t)),
        in_specs=[hbm] * 4,
        scratch_shapes=[wide, wide, flat, flat, pltpu.SemaphoreType.DMA((4,))],
        compiler_params=limit,
        name="weights",
    )(*far(b_re, b_im, decay_log, phase))
    up, init, ends = pl.pallas_call(
        lambda *refs: ends_kernel(n_tp, *refs),
        in_specs=[smem] + [vmem] * (n_tp + 2),
        out_shape=(pltpu.HBM(*rows_t), pltpu.HBM(*init_t), pltpu.HBM(*ends_t)),
        out_specs=(hbm, hbm, hbm),
        scratch_shapes=[
            held(rows_t),
            held(init_t),
            held(ends_t),
            pltpu.VMEM((total, 2 * states), F32),
            pltpu.VMEM((2 * pairs, LANES), F32),
            pltpu.SemaphoreType.DMA((3,)),
        ],
        compiler_params=limit,
        name="ends",
    )(tp_mine, *pieces, wb, tab)
    others = lax.all_to_all(ends, "sp", split_axis=0, concat_axis=0, tiled=True)
    y, cw, tab2 = pl.pallas_call(
        local_kernel,
        out_shape=(pltpu.HBM(*y_t), pltpu.VMEM(*block_t), pltpu.VMEM(*tab_t)),
        out_specs=(hbm, vmem, vmem),
        in_specs=[hbm] * 9,
        scratch_shapes=[
            held(rows_t),
            held(init_t),
            wide,
            wide,
            wide,
            wide,
            flat,
            flat,
            pltpu.VMEM((1, width), F32),
            held(y_t),
            held(block_t),
            pltpu.VMEM((total, 2 * states), F32),
            pltpu.VMEM((total, 2 * states), BF16),
            pltpu.SemaphoreType.DMA((10,)),
        ],
        compiler_params=limit,
        name="local",
    )(
        *far(
            up,
            init,
            b_re,
            b_im,
            c_real.reshape(width, entries),
            c_imag.reshape(width, entries),
            decay_log,
            phase,
            skip_gain.reshape(1, width),
        )
    )
    z = pl.pallas_call(
        carry_kernel,
        out_shape=shape(*rows_t),
        in_specs=[smem, vmem, hbm, vmem, vmem],
        scratch_shapes=[
            held(y_t),
            pltpu.VMEM((total, 2 * states), BF16),
            held(rows_t),
            pltpu.SemaphoreType.DMA,
        ],
        compiler_params=limit,
        name="carry",
    )(lax.axis_index("sp").astype(jnp.int32).reshape(1), others, *far(y), cw, tab2)
    z_all = lax.all_gather(z, "tp", axis=1, tiled=True)
    value = jnp.dot(z_all, w_value, preferred_element_type=F32)
    gate = jnp.dot(z_all, w_gate, preferred_element_type=F32)
    gated = value * jax.nn.sigmoid(gate)
    squares = jnp.sum(gated * gated, axis=1)
    m = 1
    while m < n_tp:
        squares = squares + partner(squares, m)
        m *= 2
    scale = lax.rsqrt(squares / features + NORM_EPS)
    return (gated * scale[:, None] * norm_out).astype(BF16)


def solution(mesh):
    placed = (
        P(("sp", "tp"), None),
        P(),
        P("tp", None),
        P("tp", None),
        P("tp", None, None),
        P("tp", None, None),
        P("tp", None, None),
        P("tp", None, None),
        P("tp"),
        P(None, "tp"),
        P(None, "tp"),
        P("tp"),
    )
    return jax.shard_map(on_device, mesh=mesh, in_specs=placed, out_specs=P("sp", "tp"), check_vma=False)
```
